32 devices in a mesh: ep: 8 (over z, x), tp: 4 (over y, core).
Axes of the slice: x: 2, y: 2, z: 4, core: 2. Of those that a mesh axis runs over, the one named last changes fastest.
Arguments:
- glu_value: bfloat16 [32768, 1024], P(('ep', 'tp')), may hold values from -6 to 6
- glu_gate: bfloat16 [32768, 1024], P(('ep', 'tp')), may hold values from -6 to 6
- conv_taps: float32 [31, 1024], replicated, may hold values from -12 to 12
- chan_gain: float32 [1024], replicated, may hold values from 0.1 to 1.9
- chan_shift: float32 [1024], replicated, may hold values from -3 to 3
- mix_out_weight: bfloat16 [1024, 2048], P('tp'), may hold values from -0.1875 to 0.1875
- moe_input: bfloat16 [4096, 2048], P(('ep', 'tp')), may hold values from -6 to 6
- moe_gain: float32 [2048], replicated, may hold values from 0.1 to 1.9
- expert_ids: int32 [4096, 4], P(('ep', 'tp')), may hold values from 0 to 31, all different within a row; in each aligned block of 128 rows (0 to 127, 128 to 255, ...) at most 20 rows name the same one
- expert_share: float32 [4096, 4], P(('ep', 'tp')), may hold values from 0.05 to 1
- expert_gate_weight: bfloat16 [32, 2048, 1024], P(('ep', 'tp')), may hold values from -0.375 to 0.375
- expert_up_weight: bfloat16 [32, 2048, 1024], P(('ep', 'tp')), may hold values from -0.375 to 0.375
- expert_down_weight: bfloat16 [32, 1024, 2048], P(('ep', 'tp')), may hold values from -0.0390625 to 0.0390625
Outputs:
- mixed: bfloat16 [32768, 2048], P(('ep', 'tp'))
- moe_output: bfloat16 [4096, 2048], P(('ep', 'tp'))
The draws below stay inside these ranges and needn't reach their ends.
Inputs may be any that keep to these rules, and one draw needn't show every extreme that they name: `expert_ids`: each row names 4 different experts. In each aligned block of 128 rows (the rows of one device) no expert is named by more than 20 rows, and in some block one expert is named by exactly 20 rows.
All inputs are finite; a program needn't handle non-finite values.
Results may differ from the reference program's by a relative error of at most 0.0071.
Values may be sent and summed in bfloat16 or wider, within the bound.
A program may use at most 192 MiB of HBM per device.

```python
import math
import jax
import jax.numpy as jnp
import numpy as np
from jax import lax

D = 2048
CW = 1024
KERNEL = 31
FF = 1024
TOP = 4
MOE_TOK = 128
EXPERTS = 32
CAP = 20
MIX_LEN = 32768
MOE_LEN = 4096
N_EP = 8
N_TP = 4


def draw_conv_taps(key, part):
    base_key = jax.random.fold_in(key, 11)
    tap_key, chan_key = jax.random.split(base_key)
    chan_scale = jnp.exp(jax.random.uniform(chan_key, (1, CW), jnp.float32, 0.0, 2.3))
    tap_values = jax.random.truncated_normal(tap_key, -4.0, 4.0, (KERNEL, CW), jnp.float32)
    return (tap_values * chan_scale * KERNEL ** (-0.5)).astype(jnp.float32)


def block_scale(rng, dims, shards, low, top_value):
    def one(position, blocks):
        draws = jax.random.uniform(jax.random.fold_in(jax.random.fold_in(rng, 6), position), (blocks,), jnp.float32, low / len(shards), top_value / len(shards))
        return jnp.repeat(jnp.exp(draws), dims[position] // blocks).reshape((-1,) + (1,) * (len(dims) - position - 1))

    factor_of = one(*shards[0])
    for cut in shards[1:]:
        factor_of = factor_of * one(*cut)
    return factor_of


def shared_out(own_key, own, number, rows, count, top, reach, slope):
    order = jax.random.permutation(own_key, count)
    crowded, ordinary = portions_of(count, rows * top, reach, slope, True), portions_of(count, rows * top, reach, slope, False)
    places = jnp.arange(count)

    def named(lengths, offset_by):
        used = int((lengths > 0).sum())
        fixed = max(1, used // 4)
        shifted = fixed + (places - fixed + offset_by * (used - fixed)) % max(1, count - fixed)
        return jnp.zeros((count,), jnp.int32).at[order[jnp.where(places < fixed, places, shifted)]].set(jnp.asarray(lengths, jnp.int32))

    lengths = jnp.where(number % 4 == 0, named(crowded, number // 4), named(ordinary, number - number // 4 - 1))
    mixed = jax.random.permutation(jax.random.fold_in(own, 3), count)
    source_of, sink = mixed[0:count // 2 * 2:2], mixed[1:count // 2 * 2:2]
    slack = jnp.minimum(lengths[source_of] - 1, reach - lengths[sink]) // 2
    slack = jnp.where((source_of == order[0]) | (sink == order[0]) | (lengths[sink] == 0), 0, jnp.maximum(slack, 0))
    shifted = jax.random.randint(jax.random.fold_in(own, 4), (count // 2,), 0, 1 << 20) % (slack + 1)
    lengths = lengths.at[source_of].add(-shifted).at[sink].add(shifted)
    labels = jnp.searchsorted(jnp.cumsum(lengths), jnp.arange(rows * top), side="right").astype(jnp.int32)
    listing = labels.reshape(top, rows).T
    listing = listing[jax.random.permutation(jax.random.fold_in(own, 1), rows)]
    offset_by = jax.random.randint(jax.random.fold_in(own, 2), (rows, 1), 0, top)
    return jnp.take_along_axis(listing, (jnp.arange(top)[None, :] + offset_by) % top, axis=1)


def portions_of(amount, total, reach, skew, full):
    portions = [(1 << 20) // math.isqrt(rank ** skew) + 1 for rank in range(1, amount + 1)]
    largest = reach if full else min(reach, max(-(-total // amount), total * portions[0] // sum(portions)))
    least = 1 if total - largest >= amount - 1 else 0
    given, surplus = [largest] + [least] * (amount - 1), total - largest - least * (amount - 1)
    while surplus > 0:
        movable = [i for i in range(1, amount) if given[i] < largest] or [i for i in range(1, amount) if given[i] < reach]
        pool, budget = sum([portions[i] for i in movable]), surplus
        for i in movable:
            more = min(reach - given[i], max(1, budget * portions[i] // pool), surplus)
            given[i] = given[i] + more
            surplus = surplus - more
    return np.array(given)


def centred(stream_key, dims, deviation, reach, shards=(), kind=jnp.bfloat16):
    loudness = block_scale(stream_key, dims, shards, -0.22, 0.18) if shards else 1.0
    array = jax.random.normal(stream_key, dims, jnp.float32) * deviation * loudness
    return jnp.minimum(jnp.maximum(array, -reach), reach).astype(kind)


def setup_inputs(seed: int = 0) -> dict:
    seeds = jax.random.split(jax.random.key(seed), 14)
    glu_value = centred(seeds[0], (MIX_LEN, CW), 1.0, 6.0, ((0, 32),))
    glu_gate = centred(seeds[1], (MIX_LEN, CW), 1.0, 6.0, ((0, 32),))
    conv_taps = draw_conv_taps(jax.random.fold_in(seeds[13], 71), 0)
    chan_gain = jnp.clip(1.0 + 0.18 * jax.random.normal(seeds[3], (CW,), jnp.float32), 0.1, 1.9)
    chan_shift = centred(seeds[4], (CW,), 0.5, 3.0, (), jnp.float32)
    mix_out_weight = centred(seeds[5], (CW, D), CW ** -0.5, 0.1875, ((0, 4),))
    moe_input = centred(seeds[6], (MOE_LEN, D), 1.0, 6.0, ((0, 32),))
    moe_gain = jnp.clip(1.0 + 0.18 * jax.random.normal(seeds[7], (D,), jnp.float32), 0.1, 1.9)
    expert_ids_keys = jax.random.split(jax.random.fold_in(seeds[8], 1), MOE_LEN // MOE_TOK)
    expert_ids_turns = jax.random.permutation(jax.random.fold_in(seeds[8], 3), MOE_LEN // MOE_TOK)
    expert_ids = jax.vmap(lambda own, number: shared_out(jax.random.fold_in(seeds[8], 2), own, number, MOE_TOK, EXPERTS, TOP, CAP, 1))(expert_ids_keys, expert_ids_turns).reshape((MOE_LEN, TOP))
    expert_share = jnp.clip(jnp.exp(math.log(1.0) - 2.9957323 * jax.random.uniform(seeds[9], (MOE_LEN, TOP), jnp.float32) ** block_scale(seeds[9], (MOE_LEN, TOP), ((0, 32),), -0.2, 0.2)), 0.05, 1.0)
    expert_gate_weight = centred(seeds[10], (EXPERTS, D, FF), (D // 9) ** -0.5, 0.375, ((0, 32),))
    expert_up_weight = centred(seeds[11], (EXPERTS, D, FF), (D // 9) ** -0.5, 0.375, ((0, 32),))
    expert_down_weight = centred(seeds[12], (EXPERTS, FF, D), (25 * FF) ** -0.5, 0.0390625, ((0, 32),))
    return {"glu_value": glu_value, "glu_gate": glu_gate, "conv_taps": conv_taps, "chan_gain": chan_gain, "chan_shift": chan_shift, "mix_out_weight": mix_out_weight, "moe_input": moe_input, "moe_gain": moe_gain, "expert_ids": expert_ids, "expert_share": expert_share, "expert_gate_weight": expert_gate_weight, "expert_up_weight": expert_up_weight, "expert_down_weight": expert_down_weight}


CLAMP_LIMIT = 7.0
GLU_SLOPE = 1.702

def expert_apply(flat_rows, gate_matrix, up_matrix, down_matrix):
    pre_gate = jnp.dot(flat_rows, gate_matrix, preferred_element_type=jnp.float32)
    pre_up = jnp.dot(flat_rows, up_matrix, preferred_element_type=jnp.float32)
    gated = jnp.minimum(pre_gate, CLAMP_LIMIT)
    lifted = jnp.clip(pre_up, -CLAMP_LIMIT, CLAMP_LIMIT) + 1.0
    hidden = (lifted * gated * jax.nn.sigmoid(GLU_SLOPE * gated)).astype(jnp.bfloat16)
    return jnp.dot(hidden, down_matrix, preferred_element_type=jnp.float32).astype(jnp.bfloat16)

def reference(glu_value, glu_gate, conv_taps, chan_gain, chan_shift, mix_out_weight, moe_input, moe_gain, expert_ids, expert_share, expert_gate_weight, expert_up_weight, expert_down_weight):
    gated_input = glu_value.astype(jnp.float32) * jax.nn.sigmoid(glu_gate.astype(jnp.float32))
    padded = jnp.concatenate([jnp.zeros((KERNEL - 1, CW), jnp.float32), gated_input], 0)
    convolved = jnp.zeros((MIX_LEN, CW), jnp.float32)
    for offset in range(KERNEL):
        convolved = convolved + conv_taps[offset] * padded[offset:offset + MIX_LEN]
    center = lax.optimization_barrier(jnp.mean(convolved, axis=-1, keepdims=True))
    spread = lax.optimization_barrier(jnp.mean(jnp.square(convolved - center), axis=-1, keepdims=True))
    normalized = (convolved - center) * lax.rsqrt(spread + 1e-05) * chan_gain + chan_shift
    activated = jax.nn.silu(normalized).astype(jnp.bfloat16)
    mixed = jnp.dot(activated, mix_out_weight, preferred_element_type=jnp.float32).astype(jnp.bfloat16)
    features = moe_input.astype(jnp.float32)
    scaled = features * lax.rsqrt(lax.optimization_barrier(jnp.mean(jnp.square(features), axis=-1, keepdims=True)) + 1e-06)
    moe_normed = (scaled * moe_gain).astype(jnp.bfloat16)
    flat_ids = expert_ids.reshape(-1)
    flat_share = expert_share.reshape(-1)
    slots = N_EP * N_TP * CAP

    def one_expert(total, inputs):
        number, gate_matrix, up_matrix, down_matrix = inputs
        chosen = flat_ids == number
        picked = jnp.nonzero(chosen, size=slots, fill_value=0)[0].astype(jnp.int32)
        live = jnp.arange(slots, dtype=jnp.int32) < jnp.sum(chosen.astype(jnp.int32))
        token_rows = (picked // TOP).astype(jnp.int32)
        answers = expert_apply(moe_normed[token_rows], gate_matrix, up_matrix, down_matrix)
        weights = jnp.where(live, flat_share[picked], jnp.zeros((), flat_share.dtype))
        total = total.at[token_rows].add(weights[:, None] * answers.astype(jnp.float32))
        return (total, number)
    numbers = jnp.arange(EXPERTS, dtype=jnp.int32)
    total, unused = lax.scan(one_expert, jnp.zeros((MOE_LEN, D), jnp.float32), (numbers, expert_gate_weight, expert_up_weight, expert_down_weight))
    return (mixed, total.astype(jnp.bfloat16))
```

```python
import functools

import jax
import jax.numpy as jnp
from jax import lax
from jax.experimental import pallas as pl
from jax.experimental.pallas import tpu as pltpu
from jax.sharding import PartitionSpec as P

CLAMP_LIMIT = 7.0
GLU_SLOPE = 1.702
LANES = 128
PACK = 16
MESH = pl.DeviceIdType.MESH
F32 = jnp.float32
BF16 = jnp.bfloat16


def place(flat, tp):
    return (flat // tp, flat % tp)


def greet(n, tp, me):
    barrier = pltpu.get_barrier_semaphore()

    @pl.loop(1, n)
    def _(k):
        pl.semaphore_signal(
            barrier, inc=1, device_id=place((me + k) % n, tp), device_id_type=MESH
        )

    pl.semaphore_wait(barrier, n - 1)


def slab(ref, index):
    return ref.at[pl.ds(pl.multiple_of(index * PACK, PACK), PACK)]


def exchange_copy(src, dst, ssem, rsem, me, n, tp, k):
    return pltpu.make_async_remote_copy(
        src_ref=slab(src, (me + k) % n),
        dst_ref=slab(dst, me),
        send_sem=ssem.at[k],
        recv_sem=rsem.at[k],
        device_id=place((me + k) % n, tp),
        device_id_type=MESH,
    )


def arrival(src, dst, ssem, rsem, me, n, tp, k):
    return pltpu.make_async_remote_copy(
        src_ref=slab(src, (me + k) % n),
        dst_ref=slab(dst, (me + n - k) % n),
        send_sem=ssem.at[k],
        recv_sem=rsem.at[k],
        device_id=place((me + k) % n, tp),
        device_id_type=MESH,
    )


def start_exchange(pairs, me, n, tp):
    @pl.loop(1, n)
    def _(k):
        for src, dst, ssem, rsem in pairs:
            exchange_copy(src, dst, ssem, rsem, me, n, tp, k).start()

    for src, dst, ssem, rsem in pairs:
        pltpu.make_async_copy(slab(src, me), slab(dst, me), ssem.at[0]).start()


def finish_exchange(pairs, me, n, tp):
    for src, dst, ssem, rsem in pairs:
        pltpu.make_async_copy(slab(src, me), slab(dst, me), ssem.at[0]).wait()

    @pl.loop(1, n)
    def _(k):
        for src, dst, ssem, rsem in pairs:
            copy = arrival(src, dst, ssem, rsem, me, n, tp, k)
            copy.wait_recv()
            copy.wait_send()


def first_kernel(
    n,
    tp,
    taps_count,
    margin,
    main,
    rest,
    value_all,
    gate_all,
    value,
    gate,
    taps,
    gain,
    shift,
    weight,
    main_out,
    rest_out,
    weight_out,
    act,
    halo_v,
    halo_g,
    glu,
    conv,
    main_s,
    main_r,
    rest_s,
    rest_r,
    halo_s,
    halo_r,
    weight_s,
    weight_r,
):
    step = pl.program_id(0)
    steps = pl.num_programs(0)
    e = lax.axis_index("ep")
    t = lax.axis_index("tp")
    me = e * tp + t
    rows, width = value.shape
    blocks = width // LANES
    depth = weight.shape[0]
    pairs = ((main, main_out, main_s, main_r), (rest, rest_out, rest_s, rest_r))
    positions = value_all.shape[0]

    def halo_copy(which, dest):
        src, dst = ((value_all, halo_v), (gate_all, halo_g))[which]
        return pltpu.make_async_remote_copy(
            src_ref=src.at[pl.ds(positions - margin, margin)],
            dst_ref=dst,
            send_sem=halo_s.at[which],
            recv_sem=halo_r.at[which],
            device_id=place(dest, tp),
            device_id_type=MESH,
        )

    def weight_copy(k, owner):
        return pltpu.make_async_remote_copy(
            src_ref=weight,
            dst_ref=weight_out.at[pl.ds(pl.multiple_of(owner * depth, depth), depth)],
            send_sem=weight_s.at[k],
            recv_sem=weight_r.at[k],
            device_id=(e, (t + k) % tp),
            device_id_type=MESH,
        )

    def own_weight():
        return pltpu.make_async_copy(
            weight,
            weight_out.at[pl.ds(pl.multiple_of(t * depth, depth), depth)],
            weight_s.at[0],
        )

    @pl.when(step == 0)
    def _():
        greet(n, tp, me)

        @pl.when(me < n - 1)
        def _():
            for which in range(2):
                halo_copy(which, me + 1).start()

        start_exchange(pairs, me, n, tp)
        for k in range(1, tp):
            weight_copy(k, t).start()
        own_weight().start()

        @pl.when(me > 0)
        def _():
            for which in range(2):
                halo_copy(which, me - 1).wait_recv()
            for b in range(blocks):
                cols = slice(b * LANES, (b + 1) * LANES)
                glu[b, 0:margin, :] = halo_v[:, cols].astype(F32) * jax.nn.sigmoid(
                    halo_g[:, cols].astype(F32)
                )

        @pl.when(me == 0)
        def _():
            for b in range(blocks):
                glu[b, 0:margin, :] = jnp.zeros((margin, LANES), F32)

    @pl.when(step > 0)
    def _():
        for b in range(blocks):
            glu[b, 0:margin, :] = glu[b, rows : rows + margin, :]

    for b in range(blocks):
        cols = slice(b * LANES, (b + 1) * LANES)
        glu[b, margin : margin + rows, :] = value[:, cols].astype(F32) * jax.nn.sigmoid(
            gate[:, cols].astype(F32)
        )

    part = 64
    lead = margin - (taps_count - 1)

    @pl.loop(0, rows // part)
    def _(r):
        base = r * part
        for b in range(blocks):
            cols = slice(b * LANES, (b + 1) * LANES)
            total = jnp.zeros((part, LANES), F32)
            for j in range(taps_count):
                total = total + taps[j : j + 1, cols] * glu[b, pl.ds(base + lead + j, part), :]
            conv[pl.ds(pl.multiple_of(base, part), part), cols] = total

    norm_part = 32

    @pl.loop(0, rows // norm_part)
    def _(r):
        rows_here = pl.ds(pl.multiple_of(r * norm_part, norm_part), norm_part)
        data = conv[rows_here, :]
        center = jnp.mean(data, axis=-1, keepdims=True)
        data = data - center
        spread = jnp.mean(data * data, axis=-1, keepdims=True)
        normed = data * lax.rsqrt(spread + 1e-05) * gain[...] + shift[...]
        act[rows_here, :] = (normed * jax.nn.sigmoid(normed)).astype(BF16)

    @pl.when(step == steps - 1)
    def _():
        @pl.when(me < n - 1)
        def _():
            for which in range(2):
                halo_copy(which, me + 1).wait_send()

        own_weight().wait()
        for k in range(1, tp):
            copy = weight_copy(k, (t + tp - k) % tp)
            copy.wait_recv()
            copy.wait_send()
        finish_exchange(pairs, me, n, tp)


def second_kernel(
    n, tp, main, rest, act, weight, main_out, rest_out, mixed, main_s, main_r, rest_s, rest_r
):
    step = pl.program_id(0)
    steps = pl.num_programs(0)
    me = lax.axis_index("ep") * tp + lax.axis_index("tp")
    pairs = ((main, main_out, main_s, main_r), (rest, rest_out, rest_s, rest_r))

    @pl.when(step == 0)
    def _():
        greet(n, tp, me)
        start_exchange(pairs, me, n, tp)

    mixed[...] = jnp.dot(act[...], weight[...], preferred_element_type=F32).astype(BF16)

    @pl.when(step == steps - 1)
    def _():
        finish_exchange(pairs, me, n, tp)


def fill(block):
    return pl.BlockSpec(block, lambda i: (0,) * len(block))


ANY = pl.BlockSpec(memory_space=pl.ANY)


def body(
    n,
    tp,
    glu_value,
    glu_gate,
    conv_taps,
    chan_gain,
    chan_shift,
    mix_out_weight,
    moe_input,
    moe_gain,
    expert_ids,
    expert_share,
    expert_gate_weight,
    expert_up_weight,
    expert_down_weight,
):
    tokens, per_token = expert_ids.shape
    copies = tokens * per_token
    width = moe_input.shape[1]
    capacity = max(2, 5 * copies // (4 * n))
    spare = 1
    while spare < capacity - PACK or (capacity < PACK and spare < capacity):
        spare *= 2
    has_main = capacity >= PACK
    base = PACK if has_main else 0
    cuts = PACK // spare
    piece = width // cuts
    slots = n * PACK

    features = moe_input.astype(F32)
    scaled = features * lax.rsqrt(jnp.mean(jnp.square(features), axis=-1, keepdims=True) + 1e-06)
    moe_normed = (scaled * moe_gain).astype(BF16)

    named = jnp.sum(
        (expert_ids[:, :, None] == jnp.arange(n, dtype=jnp.int32)).astype(BF16), axis=1
    )
    below = (
        jnp.arange(tokens)[:, None] > jnp.arange(tokens)[None, :]
    ).astype(BF16)
    before = jnp.dot(below, named, preferred_element_type=F32)
    hits = [
        (expert_ids[:, k : k + 1] == jnp.arange(n, dtype=jnp.int32)).astype(F32)
        for k in range(per_token)
    ]
    rank = [jnp.sum(before * hit, axis=1, keepdims=True).astype(jnp.int32) for hit in hits]
    main_code = [
        jnp.where(rank[k] < base, expert_ids[:, k : k + 1] * PACK + rank[k], -1)
        for k in range(per_token)
    ]
    rest_code = [
        jnp.where(rank[k] >= base, expert_ids[:, k : k + 1] * PACK + rank[k] - base, -slots)
        for k in range(per_token)
    ]
    lanes = jnp.arange(slots, dtype=jnp.int32)[None, :]

    def spread(codes, scales):
        total = jnp.zeros((tokens, slots), F32)
        for k in range(per_token):
            total = total + jnp.where(codes[k] == lanes, scales[k], 0.0)
        return total

    ones = [jnp.ones((tokens, 1), F32)] * per_token
    high = lax.reduce_precision(expert_share, 8, 7)
    low = expert_share - high
    highs = [high[:, k : k + 1] for k in range(per_token)]
    lows = [low[:, k : k + 1] for k in range(per_token)]

    def pick(matrix, data):
        return lax.dot_general(
            matrix, data, (((0,), (0,)), ((), ())), preferred_element_type=F32
        ).astype(BF16)

    def pieces(data):
        return jnp.concatenate([data[:, q * piece : (q + 1) * piece] for q in range(cuts)], axis=0)

    def rest_place(scales):
        return [
            spread([code + q * spare for code in rest_code], scales).astype(BF16)
            for q in range(cuts)
        ]

    if has_main:
        main = pick(spread(main_code, ones).astype(BF16), moe_normed)
    else:
        main = jnp.zeros((slots, LANES), BF16)
    rest = pick(jnp.concatenate(rest_place(ones), axis=0), pieces(moe_normed))

    positions, channels = glu_value.shape
    taps_count = conv_taps.shape[0]
    margin = -(-(taps_count - 1) // PACK) * PACK
    tile = min(256, positions)
    steps = positions // tile
    dma = pltpu.SemaphoreType.DMA
    row_tile = pl.BlockSpec((tile, channels), lambda i: (i, 0))
    out_width = mix_out_weight.shape[1]
    main_in, rest_in, weight, act = pl.pallas_call(
        functools.partial(first_kernel, n, tp, taps_count, margin),
        grid=(steps,),
        name="dispatch_and_conv",
        out_shape=(
            jax.ShapeDtypeStruct(main.shape, BF16),
            jax.ShapeDtypeStruct(rest.shape, BF16),
            jax.ShapeDtypeStruct((channels, out_width), BF16),
            jax.ShapeDtypeStruct((positions, channels), BF16),
        ),
        in_specs=[
            ANY,
            ANY,
            ANY,
            ANY,
            row_tile,
            row_tile,
            fill(conv_taps.shape),
            fill((1, channels)),
            fill((1, channels)),
            pl.BlockSpec(memory_space=pltpu.VMEM),
        ],
        out_specs=(ANY, ANY, ANY, row_tile),
        scratch_shapes=[
            pltpu.VMEM((margin, channels), BF16),
            pltpu.VMEM((margin, channels), BF16),
            pltpu.VMEM((channels // LANES, margin + tile, LANES), F32),
            pltpu.VMEM((tile, channels), F32),
            dma((n,)),
            dma((n,)),
            dma((n,)),
            dma((n,)),
            dma((2,)),
            dma((2,)),
            dma((tp,)),
            dma((tp,)),
        ],
        compiler_params=pltpu.CompilerParams(
            collective_id=0,
            has_side_effects=True,
            dimension_semantics=("arbitrary",),
            vmem_limit_bytes=32 * 1024 * 1024,
        ),
    )(
        main,
        rest,
        glu_value,
        glu_gate,
        glu_value,
        glu_gate,
        conv_taps,
        chan_gain.reshape(1, channels),
        chan_shift.reshape(1, channels),
        mix_out_weight,
    )

    row = jnp.arange(n * spare, dtype=jnp.int32)
    home = (row // spare) * PACK + row % spare
    selectors = [
        ((home + q * spare)[:, None] == jnp.arange(slots, dtype=jnp.int32)[None, :]).astype(BF16)
        for q in range(cuts)
    ]
    opened = jnp.concatenate(
        [jnp.dot(s, rest_in, preferred_element_type=F32).astype(BF16) for s in selectors], axis=1
    )
    flat_rows = jnp.concatenate([main_in, opened], axis=0) if has_main else opened
    pre_gate = jnp.dot(flat_rows, expert_gate_weight[0], preferred_element_type=F32)
    pre_up = jnp.dot(flat_rows, expert_up_weight[0], preferred_element_type=F32)
    gated = jnp.minimum(pre_gate, CLAMP_LIMIT)
    lifted = jnp.clip(pre_up, -CLAMP_LIMIT, CLAMP_LIMIT) + 1.0
    hidden = (lifted * gated * jax.nn.sigmoid(GLU_SLOPE * gated)).astype(BF16)
    answers = jnp.dot(hidden, expert_down_weight[0], preferred_element_type=F32).astype(BF16)
    if has_main:
        main_answers, rest_answers = answers[:slots], answers[slots:]
    else:
        main_answers, rest_answers = main_in, answers
    rest_answers = pick(jnp.concatenate(selectors, axis=0), pieces(rest_answers))

    main_back, rest_back, mixed = pl.pallas_call(
        functools.partial(second_kernel, n, tp),
        grid=(steps,),
        name="return_and_mix",
        out_shape=(
            jax.ShapeDtypeStruct(main.shape, BF16),
            jax.ShapeDtypeStruct(rest.shape, BF16),
            jax.ShapeDtypeStruct((positions, out_width), BF16),
        ),
        in_specs=[ANY, ANY, row_tile, fill((channels, out_width))],
        out_specs=(ANY, ANY, pl.BlockSpec((tile, out_width), lambda i: (i, 0))),
        scratch_shapes=[dma((n,)), dma((n,)), dma((n,)), dma((n,))],
        compiler_params=pltpu.CompilerParams(
            collective_id=1,
            has_side_effects=True,
            dimension_semantics=("arbitrary",),
            vmem_limit_bytes=32 * 1024 * 1024,
        ),
    )(main_answers, rest_answers, act, weight)

    def weigh(parts, data):
        both = jnp.dot(jnp.concatenate(parts, axis=0), data, preferred_element_type=F32)
        return both[:tokens] + both[tokens:]

    highs_rest, lows_rest = rest_place(highs), rest_place(lows)
    combined = jnp.concatenate(
        [weigh([highs_rest[q], lows_rest[q]], rest_back) for q in range(cuts)], axis=1
    )
    if has_main:
        combined = combined + weigh(
            [spread(main_code, highs).astype(BF16), spread(main_code, lows).astype(BF16)],
            main_back,
        )
    return (mixed, combined.astype(BF16))


def solution(mesh):
    tp = mesh.shape["tp"]
    n = mesh.shape["ep"] * tp
    both = P(("ep", "tp"), None)
    weights = P(("ep", "tp"), None, None)
    placed = (
        both, both, P(), P(), P(), P("tp", None), both, P(), both, both, weights, weights, weights
    )
    return jax.shard_map(
        functools.partial(body, n, tp),
        mesh=mesh,
        in_specs=placed,
        out_specs=(both, both),
        check_vma=False,
    )
```

```python
import functools

import jax
import jax.numpy as jnp
from jax import lax
from jax.experimental import pallas as pl
from jax.experimental.pallas import tpu as pltpu
from jax.sharding import PartitionSpec as P

CLAMP_LIMIT = 7.0
GLU_SLOPE = 1.702
LANES = 128
PACK = 16
MESH = pl.DeviceIdType.MESH
F32 = jnp.float32
BF16 = jnp.bfloat16


def place(flat, tp):
    return (flat // tp, flat % tp)


def greet(n, tp, me):
    barrier = pltpu.get_barrier_semaphore()

    @pl.loop(1, n)
    def _(k):
        pl.semaphore_signal(
            barrier, inc=1, device_id=place((me + k) % n, tp), device_id_type=MESH
        )

    pl.semaphore_wait(barrier, n - 1)


def slab(ref, index):
    return ref.at[pl.ds(pl.multiple_of(index * PACK, PACK), PACK)]


def exchange_copy(src, dst, ssem, rsem, me, n, tp, k):
    return pltpu.make_async_remote_copy(
        src_ref=slab(src, (me + k) % n),
        dst_ref=slab(dst, me),
        send_sem=ssem.at[k],
        recv_sem=rsem.at[k],
        device_id=place((me + k) % n, tp),
        device_id_type=MESH,
    )


def arrival(src, dst, ssem, rsem, me, n, tp, k):
    return pltpu.make_async_remote_copy(
        src_ref=slab(src, (me + k) % n),
        dst_ref=slab(dst, (me + n - k) % n),
        send_sem=ssem.at[k],
        recv_sem=rsem.at[k],
        device_id=place((me + k) % n, tp),
        device_id_type=MESH,
    )


def start_exchange(pairs, me, n, tp):
    @pl.loop(0, n - 1)
    def _(j):
        k = 1 + (j + n // 4 - 1) % (n - 1)
        for src, dst, ssem, rsem in pairs:
            exchange_copy(src, dst, ssem, rsem, me, n, tp, k).start()

    for src, dst, ssem, rsem in pairs:
        pltpu.make_async_copy(slab(src, me), slab(dst, me), ssem.at[0]).start()


def finish_exchange(pairs, me, n, tp):
    for src, dst, ssem, rsem in pairs:
        pltpu.make_async_copy(slab(src, me), slab(dst, me), ssem.at[0]).wait()

    @pl.loop(1, n)
    def _(k):
        for src, dst, ssem, rsem in pairs:
            copy = arrival(src, dst, ssem, rsem, me, n, tp, k)
            copy.wait_recv()
            copy.wait_send()


def first_kernel(
    n,
    tp,
    taps_count,
    margin,
    main,
    rest,
    value_all,
    gate_all,
    value,
    gate,
    taps,
    gain,
    shift,
    weight,
    main_out,
    rest_out,
    weight_out,
    act,
    halo_v,
    halo_g,
    glu,
    conv,
    main_s,
    main_r,
    rest_s,
    rest_r,
    halo_s,
    halo_r,
    weight_s,
    weight_r,
):
    step = pl.program_id(0)
    steps = pl.num_programs(0)
    e = lax.axis_index("ep")
    t = lax.axis_index("tp")
    me = e * tp + t
    rows, width = value.shape
    blocks = width // LANES
    depth = weight.shape[0]
    pairs = ((main, main_out, main_s, main_r), (rest, rest_out, rest_s, rest_r))
    positions = value_all.shape[0]

    def halo_copy(which, dest):
        src, dst = ((value_all, halo_v), (gate_all, halo_g))[which]
        return pltpu.make_async_remote_copy(
            src_ref=src.at[pl.ds(positions - margin, margin)],
            dst_ref=dst,
            send_sem=halo_s.at[which],
            recv_sem=halo_r.at[which],
            device_id=place(dest, tp),
            device_id_type=MESH,
        )

    sibling = t + 1 - 2 * (t % 2)

    def weight_rows(owner):
        return weight_out.at[pl.ds(pl.multiple_of(owner * depth, depth), depth)]

    def weight_copy(src, owner, dest, k):
        return pltpu.make_async_remote_copy(
            src_ref=src,
            dst_ref=weight_rows(owner),
            send_sem=weight_s.at[k],
            recv_sem=weight_r.at[k],
            device_id=(e, dest),
            device_id_type=MESH,
        )

    def weight_far(k, owner):
        return weight_copy(weight, owner, (t + k) % tp, k)

    def weight_relay(k):
        owner = (t + tp - k) % tp
        return weight_copy(weight_rows(owner), owner, sibling, k + 1)

    def weight_relayed(k):
        return weight_copy(weight, (sibling + tp - k) % tp, sibling, k + 1)

    def own_weight():
        return pltpu.make_async_copy(
            weight,
            weight_out.at[pl.ds(pl.multiple_of(t * depth, depth), depth)],
            weight_s.at[0],
        )

    @pl.when(step == 0)
    def _():
        greet(n, tp, me)

        @pl.when(me < n - 1)
        def _():
            for which in range(2):
                halo_copy(which, me + 1).start()

        for k in range(2, tp, 2):
            weight_far(k, t).start()
        weight_copy(weight, t, sibling, 1).start()
        start_exchange(pairs, me, n, tp)
        own_weight().start()

        @pl.when(me > 0)
        def _():
            for which in range(2):
                halo_copy(which, me - 1).wait_recv()
            for b in range(blocks):
                cols = slice(b * LANES, (b + 1) * LANES)
                glu[b, 0:margin, :] = halo_v[:, cols].astype(F32) * jax.nn.sigmoid(
                    halo_g[:, cols].astype(F32)
                )

        @pl.when(me == 0)
        def _():
            for b in range(blocks):
                glu[b, 0:margin, :] = jnp.zeros((margin, LANES), F32)

    @pl.when(step > 0)
    def _():
        for b in range(blocks):
            glu[b, 0:margin, :] = glu[b, rows : rows + margin, :]

    for b in range(blocks):
        cols = slice(b * LANES, (b + 1) * LANES)
        glu[b, margin : margin + rows, :] = value[:, cols].astype(F32) * jax.nn.sigmoid(
            gate[:, cols].astype(F32)
        )

    @pl.when(step == steps - 1)
    def _():
        for k in range(2, tp, 2):
            weight_far(k, (t + tp - k) % tp).wait_recv()
            weight_relay(k).start()

    part = 64
    lead = margin - (taps_count - 1)

    @pl.loop(0, rows // part)
    def _(r):
        base = r * part
        for b in range(blocks):
            cols = slice(b * LANES, (b + 1) * LANES)
            total = jnp.zeros((part, LANES), F32)
            for j in range(taps_count):
                total = total + taps[j : j + 1, cols] * glu[b, pl.ds(base + lead + j, part), :]
            conv[pl.ds(pl.multiple_of(base, part), part), cols] = total

    norm_part = 32

    @pl.loop(0, rows // norm_part)
    def _(r):
        rows_here = pl.ds(pl.multiple_of(r * norm_part, norm_part), norm_part)
        data = conv[rows_here, :]
        center = jnp.mean(data, axis=-1, keepdims=True)
        data = data - center
        spread = jnp.mean(data * data, axis=-1, keepdims=True)
        normed = data * lax.rsqrt(spread + 1e-05) * gain[...] + shift[...]
        act[rows_here, :] = (normed * jax.nn.sigmoid(normed)).astype(BF16)

    @pl.when(step == steps - 1)
    def _():
        @pl.when(me < n - 1)
        def _():
            for which in range(2):
                halo_copy(which, me + 1).wait_send()

        own_weight().wait()
        weight_copy(weight, sibling, sibling, 1).wait_recv()
        weight_copy(weight, t, sibling, 1).wait_send()
        for k in range(2, tp, 2):
            weight_far(k, t).wait_send()
            weight_relayed(k).wait_recv()
            weight_relay(k).wait_send()
        finish_exchange(pairs, me, n, tp)


def expert_kernel(
    has_main, n, spare, cuts, main, rest, gate, up, down, main_out, rest_out, rows, total
):
    step = pl.program_id(0)
    slots = n * PACK
    count = n * spare
    piece = main_out.shape[1] // cuts if has_main else total.shape[1] // cuts
    first = slots if has_main else 0
    bits = spare.bit_length() - 1

    def home(shape, dim, q):
        row = lax.broadcasted_iota(jnp.int32, shape, dim)
        slot = lax.broadcasted_iota(jnp.int32, shape, 1 - dim)
        where = (row >> bits) * PACK + (row & (spare - 1)) + q * spare
        return (where == slot).astype(F32).astype(BF16)

    @pl.when(step == 0)
    def _():
        if has_main:
            rows[0:slots, :] = main[...]
        for q in range(cuts):
            rows[first : first + count, q * piece : (q + 1) * piece] = jnp.dot(
                home((count, slots), 0, q), rest[...], preferred_element_type=F32
            ).astype(BF16)

    data = rows[...]
    pre_gate = jnp.dot(data, gate[0], preferred_element_type=F32)
    pre_up = jnp.dot(data, up[0], preferred_element_type=F32)
    gated = jnp.minimum(pre_gate, CLAMP_LIMIT)
    lifted = jnp.clip(pre_up, -CLAMP_LIMIT, CLAMP_LIMIT) + 1.0
    hidden = (lifted * gated * jax.nn.sigmoid(GLU_SLOPE * gated)).astype(BF16)
    part = jnp.dot(hidden, down[0], preferred_element_type=F32)

    @pl.when(step == 0)
    def _():
        total[...] = part

    @pl.when(step > 0)
    def _():
        total[...] += part

    @pl.when(step == pl.num_programs(0) - 1)
    def _():
        if has_main:
            main_out[...] = total[0:slots, :].astype(BF16)
        else:
            main_out[...] = main[...]
        folded = jnp.zeros(rest.shape, F32)
        for q in range(cuts):
            folded = folded + jnp.dot(
                home((slots, count), 1, q),
                total[first : first + count, q * piece : (q + 1) * piece].astype(BF16),
                preferred_element_type=F32,
            )
        rest_out[...] = folded.astype(BF16)


def second_kernel(
    n, tp, main, rest, act, weight, main_out, rest_out, mixed, main_s, main_r, rest_s, rest_r
):
    step = pl.program_id(0)
    steps = pl.num_programs(0)
    me = lax.axis_index("ep") * tp + lax.axis_index("tp")
    pairs = ((main, main_out, main_s, main_r), (rest, rest_out, rest_s, rest_r))

    @pl.when(step == 0)
    def _():
        greet(n, tp, me)
        start_exchange(pairs, me, n, tp)

    mixed[...] = jnp.dot(act[...], weight[...], preferred_element_type=F32).astype(BF16)

    @pl.when(step == steps - 1)
    def _():
        finish_exchange(pairs, me, n, tp)


def fill(block):
    return pl.BlockSpec(block, lambda i: (0,) * len(block))


ANY = pl.BlockSpec(memory_space=pl.ANY)


def body(
    n,
    tp,
    glu_value,
    glu_gate,
    conv_taps,
    chan_gain,
    chan_shift,
    mix_out_weight,
    moe_input,
    moe_gain,
    expert_ids,
    expert_share,
    expert_gate_weight,
    expert_up_weight,
    expert_down_weight,
):
    tokens, per_token = expert_ids.shape
    copies = tokens * per_token
    width = moe_input.shape[1]
    capacity = max(2, 5 * copies // (4 * n))
    spare = 1
    while spare < capacity - PACK or (capacity < PACK and spare < capacity):
        spare *= 2
    has_main = capacity >= PACK
    base = PACK if has_main else 0
    cuts = PACK // spare
    piece = width // cuts
    slots = n * PACK

    features = moe_input.astype(F32)
    scaled = features * lax.rsqrt(jnp.mean(jnp.square(features), axis=-1, keepdims=True) + 1e-06)
    moe_normed = (scaled * moe_gain).astype(BF16)

    named = jnp.sum(
        (expert_ids[:, :, None] == jnp.arange(n, dtype=jnp.int32)).astype(BF16), axis=1
    )
    below = (
        jnp.arange(tokens)[:, None] > jnp.arange(tokens)[None, :]
    ).astype(BF16)
    before = jnp.dot(below, named, preferred_element_type=F32)
    hits = [
        (expert_ids[:, k : k + 1] == jnp.arange(n, dtype=jnp.int32)).astype(F32)
        for k in range(per_token)
    ]
    rank = [jnp.sum(before * hit, axis=1, keepdims=True).astype(jnp.int32) for hit in hits]
    main_code = [
        jnp.where(rank[k] < base, expert_ids[:, k : k + 1] * PACK + rank[k], -1)
        for k in range(per_token)
    ]
    rest_code = [
        jnp.where(rank[k] >= base, expert_ids[:, k : k + 1] * PACK + rank[k] - base, -slots)
        for k in range(per_token)
    ]
    lanes = jnp.arange(slots, dtype=jnp.int32)[None, :]

    def spread(codes, scales):
        total = jnp.zeros((tokens, slots), F32)
        for k in range(per_token):
            total = total + jnp.where(codes[k] == lanes, scales[k], 0.0)
        return total

    ones = [jnp.ones((tokens, 1), F32)] * per_token
    high = lax.reduce_precision(expert_share, 8, 7)
    low = expert_share - high
    highs = [high[:, k : k + 1] for k in range(per_token)]
    lows = [low[:, k : k + 1] for k in range(per_token)]

    def pick(matrix, data):
        return lax.dot_general(
            matrix, data, (((0,), (0,)), ((), ())), preferred_element_type=F32
        ).astype(BF16)

    def pieces(data):
        return jnp.concatenate([data[:, q * piece : (q + 1) * piece] for q in range(cuts)], axis=0)

    def rest_place(scales):
        return [
            spread([code + q * spare for code in rest_code], scales).astype(BF16)
            for q in range(cuts)
        ]

    if has_main:
        main = pick(spread(main_code, ones).astype(BF16), moe_normed)
    else:
        main = jnp.zeros((slots, LANES), BF16)
    rest = pick(jnp.concatenate(rest_place(ones), axis=0), pieces(moe_normed))

    positions, channels = glu_value.shape
    taps_count = conv_taps.shape[0]
    margin = -(-(taps_count - 1) // PACK) * PACK
    tile = min(256, positions)
    steps = positions // tile
    dma = pltpu.SemaphoreType.DMA
    row_tile = pl.BlockSpec((tile, channels), lambda i: (i, 0))
    out_width = mix_out_weight.shape[1]
    main_in, rest_in, weight, act = pl.pallas_call(
        functools.partial(first_kernel, n, tp, taps_count, margin),
        grid=(steps,),
        name="dispatch_and_conv",
        out_shape=(
            jax.ShapeDtypeStruct(main.shape, BF16),
            jax.ShapeDtypeStruct(rest.shape, BF16),
            jax.ShapeDtypeStruct((channels, out_width), BF16),
            jax.ShapeDtypeStruct((positions, channels), BF16),
        ),
        in_specs=[
            ANY,
            ANY,
            ANY,
            ANY,
            row_tile,
            row_tile,
            fill(conv_taps.shape),
            fill((1, channels)),
            fill((1, channels)),
            pl.BlockSpec(memory_space=pltpu.VMEM),
        ],
        out_specs=(ANY, ANY, ANY, row_tile),
        scratch_shapes=[
            pltpu.VMEM((margin, channels), BF16),
            pltpu.VMEM((margin, channels), BF16),
            pltpu.VMEM((channels // LANES, margin + tile, LANES), F32),
            pltpu.VMEM((tile, channels), F32),
            dma((n,)),
            dma((n,)),
            dma((n,)),
            dma((n,)),
            dma((2,)),
            dma((2,)),
            dma((tp,)),
            dma((tp,)),
        ],
        compiler_params=pltpu.CompilerParams(
            collective_id=0,
            has_side_effects=True,
            dimension_semantics=("arbitrary",),
            vmem_limit_bytes=32 * 1024 * 1024,
        ),
    )(
        main,
        rest,
        glu_value,
        glu_gate,
        glu_value,
        glu_gate,
        conv_taps,
        chan_gain.reshape(1, channels),
        chan_shift.reshape(1, channels),
        mix_out_weight,
    )

    hidden_units = expert_gate_weight.shape[2]
    block = min(256, hidden_units)
    count = (slots if has_main else 0) + n * spare
    columns = pl.BlockSpec((1, width, block), lambda f: (0, 0, f))
    main_answers, rest_answers = pl.pallas_call(
        functools.partial(expert_kernel, has_main, n, spare, cuts),
        grid=(hidden_units // block,),
        name="experts",
        out_shape=(
            jax.ShapeDtypeStruct(main.shape, BF16),
            jax.ShapeDtypeStruct(rest.shape, BF16),
        ),
        in_specs=[
            fill(main.shape),
            fill(rest.shape),
            columns,
            columns,
            pl.BlockSpec((1, block, width), lambda f: (0, f, 0)),
        ],
        out_specs=(fill(main.shape), fill(rest.shape)),
        scratch_shapes=[pltpu.VMEM((count, width), BF16), pltpu.VMEM((count, width), F32)],
        compiler_params=pltpu.CompilerParams(
            dimension_semantics=("arbitrary",), vmem_limit_bytes=44 * 1024 * 1024
        ),
    )(main_in, rest_in, expert_gate_weight, expert_up_weight, expert_down_weight)

    main_back, rest_back, mixed = pl.pallas_call(
        functools.partial(second_kernel, n, tp),
        grid=(steps,),
        name="return_and_mix",
        out_shape=(
            jax.ShapeDtypeStruct(main.shape, BF16),
            jax.ShapeDtypeStruct(rest.shape, BF16),
            jax.ShapeDtypeStruct((positions, out_width), BF16),
        ),
        in_specs=[ANY, ANY, row_tile, fill((channels, out_width))],
        out_specs=(ANY, ANY, pl.BlockSpec((tile, out_width), lambda i: (i, 0))),
        scratch_shapes=[dma((n,)), dma((n,)), dma((n,)), dma((n,))],
        compiler_params=pltpu.CompilerParams(
            collective_id=1,
            has_side_effects=True,
            dimension_semantics=("arbitrary",),
            vmem_limit_bytes=32 * 1024 * 1024,
        ),
    )(main_answers, rest_answers, act, weight)

    def weigh(parts, data):
        both = jnp.dot(jnp.concatenate(parts, axis=0), data, preferred_element_type=F32)
        return both[:tokens] + both[tokens:]

    highs_rest, lows_rest = rest_place(highs), rest_place(lows)
    combined = jnp.concatenate(
        [weigh([highs_rest[q], lows_rest[q]], rest_back) for q in range(cuts)], axis=1
    )
    if has_main:
        combined = combined + weigh(
            [spread(main_code, highs).astype(BF16), spread(main_code, lows).astype(BF16)],
            main_back,
        )
    return (mixed, combined.astype(BF16))


def solution(mesh):
    tp = mesh.shape["tp"]
    n = mesh.shape["ep"] * tp
    both = P(("ep", "tp"), None)
    weights = P(("ep", "tp"), None, None)
    placed = (
        both, both, P(), P(), P(), P("tp", None), both, P(), both, both, weights, weights, weights
    )
    return jax.shard_map(
        functools.partial(body, n, tp),
        mesh=mesh,
        in_specs=placed,
        out_specs=(both, both),
        check_vma=False,
    )
```
